256 devices in a mesh: sp: 32 (over z, y), fs: 4 (over x), tp: 2 (over core).
Axes of the slice: x: 4, y: 4, z: 8, core: 2. Of those that a mesh axis runs over, the one named last changes fastest.
Arguments:
- tokens: bfloat16 [4, 8192, 2048], P('fs', ('sp', 'tp')), may hold values from -6 to 6
- norm_gain: float32 [2048], replicated, may hold values from 0.1 to 1.9
- w_conv_gate: bfloat16 [2048, 1024], P('sp', 'tp'), may hold values from -0.125 to 0.125
- w_conv_in: bfloat16 [2048, 1024], P('sp', 'tp'), may hold values from -0.125 to 0.125
- w_conv_value: bfloat16 [2048, 1024], P('sp', 'tp'), may hold values from -0.125 to 0.125
- conv_taps: float32 [3, 1024], P(None, 'tp'), may hold values from -3.5 to 3.5
- w_receptance: bfloat16 [2048, 1024], P('sp', 'tp'), may hold values from -0.125 to 0.125
- w_key: bfloat16 [2048, 1024], P('sp', 'tp'), may hold values from -0.125 to 0.125
- w_value: bfloat16 [2048, 1024], P('sp', 'tp'), may hold values from -0.125 to 0.125
- w_decay_down: bfloat16 [2048, 128], P('sp'), may hold values from -0.125 to 0.125
- w_decay_up: bfloat16 [128, 1024], P(None, 'tp'), may hold values from -0.75 to 0.75
- decay_base: float32 [1024], P('tp'), may hold values from -12.5 to -3
- decay_shift: float32 [4, 8192, 1024], P('fs', 'sp', 'tp'), may hold values from -2.1 to 0
- w_rate_down: bfloat16 [2048, 128], P('sp'), may hold values from -0.125 to 0.125
- w_rate_up: bfloat16 [128, 1024], P(None, 'tp'), may hold values from -0.5 to 0.5
- rate_base: float32 [1024], P('tp'), may hold values from -10 to 1
- key_scale: float32 [1024], P('tp'), may hold values from 0.25 to 2.5
- key_mix: float32 [1024], P('tp'), may hold values from 0.1 to 0.7
- group_gain: float32 [1024], P('tp'), may hold values from 0.1 to 1.9
- w_out_conv: bfloat16 [1024, 2048], P('tp', 'sp'), may hold values from -0.125 to 0.125
- w_out_state: bfloat16 [1024, 2048], P('tp', 'sp'), may hold values from -0.125 to 0.125
Outputs:
- mixed: bfloat16 [4, 8192, 2048], P('fs', ('sp', 'tp'))
The draws below stay inside these ranges and needn't reach their ends.
All inputs are finite; a program needn't handle non-finite values.
Results may differ from the reference program's by a relative error of at most 0.015.
Values may be sent and summed in bfloat16 or wider, within the bound.
A program may use at most 128 MiB of HBM per device.

```python
import math
import jax
import jax.numpy as jnp
from jax import lax

D = 2048
CONV_CH = 1024
HEADS = 16
HEAD = 64
DECAY_RANK = 128
RATE_RANK = 128
TOK_DEV = 256
STATE_CH = 1024
SERIES_STEPS = 8192
BATCH_SERIES = 4
N_TP = 2


def quick_head_count(key):
    head_count = STATE_CH // HEAD
    order = jax.random.permutation(jax.random.fold_in(key, 101), head_count)
    chosen = order < head_count // 2
    return jnp.repeat(chosen, HEAD)


def draw_decay_base(key, part):
    jitter = jax.random.uniform(jax.random.fold_in(key, 202), (STATE_CH,), jnp.float32, -0.5, 0.5)
    return jnp.where(quick_head_count(key), -3.5 + jitter, -12.0 + jitter)


def draw_rate_base(key, part):
    quick = jax.random.uniform(jax.random.fold_in(key, 303), (STATE_CH,), jnp.float32, -1.0, 1.0)
    slower = jax.random.uniform(jax.random.fold_in(key, 404), (STATE_CH,), jnp.float32, -10.0, -8.0)
    return jnp.where(quick_head_count(key), quick, slower)


def draw_decay_shift(key, part):
    block_count = SERIES_STEPS // TOK_DEV
    levels = jnp.exp(jax.random.uniform(jax.random.fold_in(key, 505), (BATCH_SERIES, block_count, 1, 1), jnp.float32, math.log(3e-06), math.log(6e-05)))
    rough = jnp.exp(jax.random.uniform(jax.random.fold_in(key, 606), (BATCH_SERIES, block_count, TOK_DEV, STATE_CH), jnp.float32, math.log(0.5), math.log(2.0)))
    drift = -(levels * rough).reshape(BATCH_SERIES, SERIES_STEPS, STATE_CH)
    spike_location = jax.random.randint(jax.random.fold_in(key, 707), (BATCH_SERIES, 3), 0, SERIES_STEPS)
    losses = jnp.log(jax.random.uniform(jax.random.fold_in(key, 808), (BATCH_SERIES, 3, STATE_CH), jnp.float32, 0.5, 0.8))
    slot_numbers = jnp.arange(SERIES_STEPS)
    spike_total = (slot_numbers[None, None, :] == spike_location[:, :, None]).astype(jnp.float32)
    return drift + jnp.einsum('sbl,sbc->slc', spike_total, losses)


def level_of(key, dims, split, low, high):
    loudness, own = 1.0, jax.random.fold_in(key, 6)
    for dim, blocks in split:
        heights = jnp.exp(jax.random.uniform(jax.random.fold_in(own, dim), (blocks,), jnp.float32, low / len(split), high / len(split)))
        loudness = loudness * jnp.repeat(heights, dims[dim] // blocks).reshape([-1 if axis == dim else 1 for axis in range(len(dims))])
    return loudness


def scatter_about(rng, extent, width, bound, cuts=(), kind=jnp.bfloat16):
    factor_of = level_of(rng, extent, cuts, -0.22, 0.18) if cuts else 1.0
    entries = jax.random.normal(rng, extent, jnp.float32) * width * factor_of
    return jnp.minimum(jnp.maximum(entries, -bound), bound).astype(kind)


def setup_inputs(seed: int = 0) -> dict:
    streams_of = jax.random.split(jax.random.key(seed), 22)
    return {
        "tokens": scatter_about(streams_of[0], (BATCH_SERIES, SERIES_STEPS, D), 1.0, 6.0, ((0, 4), (1, 64))),
        "norm_gain": jnp.clip(1.0 + 0.18 * jax.random.normal(streams_of[1], (D,), jnp.float32), 0.1, 1.9),
        "w_conv_gate": scatter_about(streams_of[2], (D, CONV_CH), D ** -0.5, 0.125, ((0, 32), (1, 2))),
        "w_conv_in": scatter_about(streams_of[3], (D, CONV_CH), D ** -0.5, 0.125, ((0, 32), (1, 2))),
        "w_conv_value": scatter_about(streams_of[4], (D, CONV_CH), D ** -0.5, 0.125, ((0, 32), (1, 2))),
        "conv_taps": scatter_about(streams_of[5], (3, CONV_CH), 3 ** -0.5, 3.5, ((1, 2),), jnp.float32),
        "w_receptance": scatter_about(streams_of[6], (D, STATE_CH), D ** -0.5, 0.125, ((0, 32), (1, 2))),
        "w_key": scatter_about(streams_of[7], (D, STATE_CH), D ** -0.5, 0.125, ((0, 32), (1, 2))),
        "w_value": scatter_about(streams_of[8], (D, STATE_CH), D ** -0.5, 0.125, ((0, 32), (1, 2))),
        "w_decay_down": scatter_about(streams_of[9], (D, DECAY_RANK), D ** -0.5, 0.125, ((0, 32),)),
        "w_decay_up": scatter_about(streams_of[10], (DECAY_RANK, STATE_CH), (DECAY_RANK // 2) ** -0.5, 0.75, ((1, 2),)),
        "decay_base": draw_decay_base(jax.random.fold_in(streams_of[21], 71), 0),
        "decay_shift": draw_decay_shift(jax.random.fold_in(streams_of[21], 71), 0),
        "w_rate_down": scatter_about(streams_of[13], (D, RATE_RANK), D ** -0.5, 0.125, ((0, 32),)),
        "w_rate_up": scatter_about(streams_of[14], (RATE_RANK, STATE_CH), RATE_RANK ** -0.5, 0.5, ((1, 2),)),
        "rate_base": draw_rate_base(jax.random.fold_in(streams_of[21], 71), 0),
        "key_scale": jnp.clip(jnp.exp(math.log(2.5) - 2.3025851 * jax.random.uniform(streams_of[16], (STATE_CH,), jnp.float32) ** level_of(streams_of[16], (STATE_CH,), ((0, 2),), -0.2, 0.2)), 0.25, 2.5),
        "key_mix": jnp.clip(0.1 + 0.59999999 * jax.random.uniform(streams_of[17], (STATE_CH,), jnp.float32) ** level_of(streams_of[17], (STATE_CH,), ((0, 2),), -0.2, 0.2), 0.1, 0.7),
        "group_gain": jnp.clip(1.0 + 0.18 * jax.random.normal(streams_of[18], (STATE_CH,), jnp.float32), 0.1, 1.9),
        "w_out_conv": scatter_about(streams_of[19], (CONV_CH, D), (CONV_CH + STATE_CH) ** -0.5, 0.125, ((0, 2), (1, 32))),
        "w_out_state": scatter_about(streams_of[20], (STATE_CH, D), (CONV_CH + STATE_CH) ** -0.5, 0.125, ((0, 2), (1, 32))),
    }


highest = lax.Precision.HIGHEST

def normalize_rows(rows_in, norm_gain):
    values = rows_in.astype(jnp.float32)
    scaled = values * lax.rsqrt(lax.optimization_barrier(jnp.mean(values * values, axis=-1, keepdims=True)) + 1e-06)
    return (scaled * norm_gain).astype(jnp.bfloat16)

def project(normed, weight):
    return jnp.dot(normed, weight, preferred_element_type=jnp.float32).astype(jnp.bfloat16)

def recurrence(receptance, decay_mul, key_write, value_vec, erase_vec, replace_vec):

    def advance(memory, inputs_now):
        recv_now, decay_now, key_now, value_now, erase_now, replace_now = inputs_now
        erased = jnp.einsum('hvk,hk->hv', memory, erase_now, precision=highest)
        memory = memory * decay_now[:, None, :] + erased[:, :, None] * replace_now[:, None, :] + value_now[:, :, None] * key_now[:, None, :]
        return (memory, jnp.einsum('hvk,hk->hv', memory, recv_now, precision=highest))
    initial = jnp.zeros((HEADS, HEAD, HEAD), jnp.float32)
    return lax.scan(advance, initial, (receptance, decay_mul, key_write, value_vec, erase_vec, replace_vec))[1]

def merge_outputs(conv_out, state_out, w_out_conv, w_out_state):
    filter_branch_output = CONV_CH // N_TP
    state_part = STATE_CH // N_TP
    combined = jnp.zeros((conv_out.shape[0], w_out_conv.shape[1]), jnp.float32)
    for member in range(N_TP):
        conv_lo = member * filter_branch_output
        state_lo = member * state_part
        partial_sum = jnp.dot(conv_out[:, conv_lo:conv_lo + filter_branch_output], w_out_conv[conv_lo:conv_lo + filter_branch_output], preferred_element_type=jnp.float32) + jnp.dot(state_out[:, state_lo:state_lo + state_part], w_out_state[state_lo:state_lo + state_part], preferred_element_type=jnp.float32)
        rounded = lax.optimization_barrier(partial_sum.astype(jnp.bfloat16))
        combined = combined + rounded.astype(jnp.float32)
    return combined.astype(jnp.bfloat16)

def split_heads(values):
    return values.reshape(values.shape[0], HEADS, HEAD)

def reference(tokens, norm_gain, w_conv_gate, w_conv_in, w_conv_value, conv_taps, w_receptance, w_key, w_value, w_decay_down, w_decay_up, decay_base, decay_shift, w_rate_down, w_rate_up, rate_base, key_scale, key_mix, group_gain, w_out_conv, w_out_state):
    results = []
    for sequence in range(BATCH_SERIES):
        normed = normalize_rows(tokens[sequence], norm_gain)
        conv_gate = project(normed, w_conv_gate)
        filter_source = project(normed, w_conv_in)
        conv_value = project(normed, w_conv_value)
        product_value = filter_source.astype(jnp.float32) * conv_value.astype(jnp.float32)
        padded = jnp.concatenate([jnp.zeros((2, CONV_CH), jnp.float32), product_value], axis=0)
        filtered = conv_taps[0] * padded[:-2] + conv_taps[1] * padded[1:-1] + conv_taps[2] * padded[2:]
        conv_out = (conv_gate.astype(jnp.float32) * filtered).astype(jnp.bfloat16)
        receptance = project(normed, w_receptance)
        key_raw = project(normed, w_key)
        value_raw = project(normed, w_value)
        decay_low = project(normed, w_decay_down)
        rate_low = project(normed, w_rate_down)
        decay_act = jnp.tanh(decay_low.astype(jnp.float32)).astype(jnp.bfloat16)
        decay_pre = decay_base + jnp.dot(decay_act, w_decay_up, preferred_element_type=jnp.float32)
        log_decay = decay_shift[sequence] - jnp.exp(-jax.nn.softplus(-decay_pre) - 0.5)
        learn_rate = jax.nn.sigmoid(rate_base + jnp.dot(rate_low, w_rate_up, preferred_element_type=jnp.float32))
        scaled_key = split_heads(key_raw.astype(jnp.float32) * key_scale)
        erase_dir = scaled_key * lax.rsqrt(lax.optimization_barrier(jnp.sum(scaled_key * scaled_key, axis=-1, keepdims=True)) + 1e-06)
        key_write = key_raw.astype(jnp.float32) * (1.0 + (learn_rate - 1.0) * key_mix)
        readouts = recurrence(split_heads(receptance.astype(jnp.float32)), split_heads(jnp.exp(log_decay)), split_heads(key_write), split_heads(value_raw.astype(jnp.float32)), -erase_dir, erase_dir * split_heads(learn_rate))
        centered = readouts - lax.optimization_barrier(jnp.mean(readouts, axis=-1, keepdims=True))
        variance = lax.optimization_barrier(jnp.mean(centered * centered, axis=-1, keepdims=True))
        normal_heads = (centered * lax.rsqrt(variance + 0.00064)).reshape(SERIES_STEPS, STATE_CH)
        state_out = (normal_heads * group_gain).astype(jnp.bfloat16)
        results.append(merge_outputs(conv_out, state_out, w_out_conv, w_out_state))
    return jnp.stack(results)
```

```python
import jax
import jax.numpy as jnp
from jax import lax
from jax.experimental import pallas as pl
from jax.experimental.pallas import tpu as pltpu
from jax.sharding import Mesh
from jax.sharding import PartitionSpec as P

MESH = pl.DeviceIdType.MESH
AXES = ("sp_0", "sp_1", "fs", "tp")
SP = ("sp_0", "sp_1")
SP_TP = ("sp_0", "sp_1", "tp")
NZ, NY, NX = 8, 4, 4
HEAD = 64
LANES = 128
BLOCK = 64
COLS_IN = 7 * LANES
COLS = 9 * LANES
F32, BF16 = jnp.float32, jnp.bfloat16
norm_eps = 1e-06
group_eps = 0.00064


def here():
    return tuple(lax.axis_index(a) for a in AXES)


def enter(peers):
    barrier = pltpu.get_barrier_semaphore()
    for peer in peers:
        pl.semaphore_signal(barrier, inc=1, device_id=peer, device_id_type=MESH)
    return lambda: pl.semaphore_wait(barrier, len(peers))


def remote(src, dst, send_sem, recv_sem, peer):
    return pltpu.make_async_remote_copy(
        src_ref=src, dst_ref=dst, send_sem=send_sem, recv_sem=recv_sem, device_id=peer, device_id_type=MESH
    )


def gather_kernel(
    tok_ref, gain_ref, wp_ref, shift_ref,
    proj_ref, low_ref, shift_out, wout_ref,
    T, W, DS, LOW,
    w_send, w_recv, a_send, a_recv, s_send, s_recv, t_send, t_recv, c_send, c_recv, l_send, l_recv,
):
    z, y, x, c = here()

    def at(dz=0, dy=0, dx=0, dc=0):
        return (lax.rem(z + dz, NZ), lax.rem(y + dy, NY), lax.rem(x + dx, NX), lax.rem(c + dc, 2))

    peers = [at(dz=1), at(dz=7), at(dx=1), at(dx=3), at(dy=1), at(dy=2), at(dy=3), at(dc=1)]
    entered = enter(peers)
    x16 = pl.multiple_of(x * 16, 16)
    lane_of = lambda yy: pl.ds(pl.multiple_of(yy * LANES, LANES), LANES)
    W[z, y, x] = wp_ref[y, pl.ds(x16, 16), :]
    DS[y] = shift_ref[:, lane_of(y)]
    gain = gain_ref[...]

    @pl.loop(0, 4)
    def _(i):
        rows = pl.ds(pl.multiple_of(i * 32, 32), 32)
        values = tok_ref[rows, :].astype(F32)
        scaled = values * lax.rsqrt(jnp.mean(values * values, axis=-1, keepdims=True) + norm_eps)
        T[y, c, rows, :] = (scaled * gain).astype(BF16)

    entered()
    waits = []

    def go(copy):
        copy.start()
        waits.append(copy)
        return copy

    arrive_a = []
    for d in (1, 3, 2):
        to = lax.rem(y + d, NY)
        arrive_a.append(go(remote(wp_ref.at[to, pl.ds(x16, 16), :], W.at[z, y, x], a_send.at[d - 1], a_recv.at[d - 1], at(dy=d))))
    def token_unit(dy, half):
        return T.at[lax.rem(y + NY - dy, NY), c, pl.ds(half * 64, 64), :]

    def token_send(dy, half, to_dy, via):
        k = to_dy * 2 + half
        return go(remote(token_unit(dy, half), token_unit(dy, half), t_send.at[k], t_recv.at[k], at(dy=via)))

    t10 = token_send(0, 0, 1, 1)
    t31 = token_send(0, 1, 3, 3)
    t11 = token_send(0, 1, 1, 1)
    t30 = token_send(0, 0, 3, 3)
    other = at(dc=1)

    def across(dy):
        unit = T.at[lax.rem(y + NY - dy, NY), c]
        return go(remote(unit, unit, c_send.at[dy], c_recv.at[dy], other))

    crossed = [across(0)]
    for d in (1, 3, 2):
        to = lax.rem(y + d, NY)
        go(remote(shift_ref.at[:, lane_of(to)], DS.at[y], s_send.at[d - 1], s_recv.at[d - 1], at(dy=d)))

    def unit(h, dz, dx):
        return W.at[lax.rem(z + NZ - dz, NZ), pl.ds(2 * h, 2), lax.rem(x + NX - dx, NX)]

    copies = {}

    def send(h, dz, dx, step_z, step_x):
        nz, nx = (dz + step_z) % NZ, (dx + step_x) % NX
        copies[h, nz, nx] = go(
            remote(unit(h, dz, dx), unit(h, dz, dx), w_send.at[h, nz, nx], w_recv.at[h, nz, nx], at(dz=step_z % NZ, dx=step_x % NX))
        )

    def forward(h, dz, dx):
        if h == 0:
            if dx == 0:
                if dz in (0, 1, 2, 3):
                    send(0, dz, 0, 1, 0)
                if dz in (0, 7, 6):
                    send(0, dz, 0, -1, 0)
                send(0, dz, 0, 0, 1)
                send(0, dz, 0, 0, -1)
            elif dx == 1 and dz % 2 == 0:
                send(0, dz, 1, 0, 1)
            elif dx == 3 and dz % 2 == 1:
                send(0, dz, 3, 0, -1)
        else:
            if dz == 0:
                if dx in (0, 1):
                    send(1, 0, dx, 0, 1)
                if dx == 0:
                    send(1, 0, dx, 0, -1)
                send(1, 0, dx, 1, 0)
                send(1, 0, dx, -1, 0)
            elif dz in (1, 2) or (dz == 3 and dx % 2 == 0):
                send(1, dz, dx, 1, 0)
            elif dz in (7, 6) or (dz == 5 and dx % 2 == 1):
                send(1, dz, dx, -1, 0)

    def hops(h, dz, dx):
        return min(dz, NZ - dz) + min(dx, NX - dx)

    for copy in arrive_a:
        copy.wait_recv()
    order = sorted(
        ((h, dz, dx) for h in range(2) for dz in range(NZ) for dx in range(NX)),
        key=lambda u: (hops(*u), u[0], min(u[2], NX - u[2]), u[1]),
    )
    token_at = 12
    for k, u in enumerate(order):
        if k >= 2:
            copies[u].wait_recv()
        forward(*u)
        if k == token_at:
            t10.wait_recv()
            t20 = token_send(1, 0, 2, 1)
            t31.wait_recv()
            t21 = token_send(3, 1, 2, 3)
        if k == token_at + 16:
            t11.wait_recv()
            t30.wait_recv()
            crossed += [across(1), across(3)]
    t20.wait_recv()
    t21.wait_recv()
    crossed.append(across(2))
    for copy in crossed:
        copy.wait_recv()

    def rows_of(i):
        return T[i].reshape(256, 2048)

    @pl.loop(0, NY)
    def _(i):
        w = W[:, :, :, :, 6 * LANES : 7 * LANES].reshape(2048, LANES)
        out = jnp.dot(rows_of(i), w, preferred_element_type=F32)
        LOW[c, pl.ds(pl.multiple_of(i * 256, 256), 256), :] = out.astype(BF16)

    low_copy = remote(LOW.at[c], LOW.at[c], l_send.at[0], l_recv.at[0], other)
    low_copy.start()

    @pl.loop(0, NY)
    def _(i):
        rows = pl.ds(pl.multiple_of(i * 256, 256), 256)
        for n in range(3):
            w = W[:, :, :, :, n * 256 : n * 256 + 256].reshape(2048, 256)
            out = jnp.dot(rows_of(i), w, preferred_element_type=F32)
            proj_ref[rows, n * 256 : n * 256 + 256] = out.astype(BF16)

    wout_ref[...] = W[:, :, :, :, 7 * LANES :].reshape(2048, 256)
    for d in (1, 2, 3):
        to = lax.rem(y + d, NY)
        remote(shift_ref.at[:, lane_of(to)], DS.at[y], s_send.at[d - 1], s_recv.at[d - 1], at(dy=d)).wait_recv()
    shift_out[...] = DS[...].reshape(1024, LANES)
    low_copy.wait_recv()
    low_ref[...] = LOW[...]
    low_copy.wait_send()
    for copy in waits:
        copy.wait_send()


def gather_and_project(tokens, gain, wp, shift):
    vmem = pl.BlockSpec(memory_space=pltpu.VMEM)
    dma = pltpu.SemaphoreType.DMA
    return pl.pallas_call(
        gather_kernel,
        name="gather_project",
        out_shape=(
            jax.ShapeDtypeStruct((1024, 6 * LANES), BF16),
            jax.ShapeDtypeStruct((2, 1024, LANES), BF16),
            jax.ShapeDtypeStruct((1024, LANES), F32),
            jax.ShapeDtypeStruct((2048, 2 * LANES), BF16),
        ),
        in_specs=[vmem] * 4,
        out_specs=(vmem,) * 4,
        scratch_shapes=[
            pltpu.VMEM((NY, 2, 128, 2048), BF16),
            pltpu.VMEM((NZ, NY, NX, 16, COLS), BF16),
            pltpu.VMEM((NY, 256, LANES), F32),
            pltpu.VMEM((2, 1024, LANES), BF16),
            dma((2, NZ, NX)), dma((2, NZ, NX)), dma((3,)), dma((3,)), dma((3,)), dma((3,)),
            dma((8,)), dma((8,)), dma((4,)), dma((4,)), dma((1,)), dma((1,)),
        ],
        compiler_params=pltpu.CompilerParams(collective_id=1, has_side_effects=True, vmem_limit_bytes=48 << 20),
        cost_estimate=pl.CostEstimate(flops=4_000_000_000, bytes_accessed=16_000_000, transcendentals=0),
    )(tokens, gain, wp, shift)


def halves(a):
    high = a.astype(BF16)
    return high, (a - high.astype(F32)).astype(BF16)


def dot(a, b):
    return jnp.dot(a, b, preferred_element_type=F32)


def dot_nt(a, b):
    return lax.dot_general(a, b, (((1,), (1,)), ((), ())), preferred_element_type=F32)


def mm(a, b):
    ah, al = halves(a)
    bh, bl = halves(b)
    both = jnp.concatenate([bh, bl], axis=1)
    out = dot(jnp.concatenate([ah, al], axis=1), jnp.concatenate([both, both], axis=0))
    return out[:, :LANES] + out[:, LANES:]


def mm_wide(a, b):
    ah, al = halves(a)
    bh, bl = halves(b)
    return dot(jnp.concatenate([ah, al], axis=1), jnp.concatenate([bh, bh], axis=0)) + dot(ah, bl)


def mm_nt_wide(a, b):
    ah, al = halves(a)
    bh, bl = halves(b)
    return dot_nt(jnp.concatenate([ah, al], axis=1), jnp.concatenate([bh, bh], axis=1)) + dot_nt(ah, bl)


def head_sum(values, ones):
    high, low = halves(values)
    return dot(high, ones) + dot(low, ones)


def block_kernel(
    y_param, proj_ref, low_ref, shift_ref, up_d_ref, up_r_ref, par_ref,
    qp_ref, loc_ref, gh_ref,
    LD, AD, BD, KW, GC, QM, LO, X,
):
    y = lax.axis_index("sp_1")
    mine = pl.ds(pl.multiple_of(y * LANES, LANES), LANES)
    lane = lax.broadcasted_iota(jnp.int32, (128, LANES), 1)
    row = lax.broadcasted_iota(jnp.int32, (128, LANES), 0)
    same_head = (row // HEAD) == (lane // HEAD)
    ones = jnp.where(same_head, 1.0, 0.0).astype(BF16)
    up_d, up_r = up_d_ref[:, mine], up_r_ref[:, mine]
    decay_base, rate_base = par_ref[0:1, mine], par_ref[1:2, mine]
    key_scale, key_mix = par_ref[2:3, mine], par_ref[3:4, mine]

    @pl.loop(0, 4)
    def _(i):
        rows = pl.ds(pl.multiple_of(i * 256, 256), 256)
        act = jnp.tanh(low_ref[0, rows, :].astype(F32)).astype(BF16)
        pre = decay_base + dot(act, up_d)
        LD[rows, :] = shift_ref[rows, :] - jax.nn.sigmoid(pre) * 0.6065306597126334
        rate = jax.nn.sigmoid(rate_base + dot(low_ref[1, rows, :], up_r))
        key = proj_ref[rows, 4 * LANES : 5 * LANES].astype(F32)
        scaled = key * key_scale
        erase = scaled * lax.rsqrt(head_sum(scaled * scaled, ones) + norm_eps)
        AD[rows, :] = -erase
        BD[rows, :] = erase * rate
        KW[rows, :] = key * (1.0 + (rate - 1.0) * key_mix)

    t, s = row % HEAD, lane % HEAD
    strict = same_head & (t > s)
    causal = same_head & (t >= s)
    same32 = (t // 32) == (s // 32)
    eye = jnp.where(row == lane, 1.0, 0.0)
    offs = {
        b: same_head & ((t // (2 * b)) == (s // (2 * b))) & ((t // b) % 2 == 1) & ((s // b) % 2 == 0) for b in (1, 2, 4, 8, 16, 32)
    }
    low64 = lax.broadcasted_iota(jnp.int32, (BLOCK, LANES), 1) < HEAD
    row64 = lax.broadcasted_iota(jnp.int32, (BLOCK, LANES), 0)
    tri = jnp.where(
        lax.broadcasted_iota(jnp.int32, (BLOCK, BLOCK), 0) >= lax.broadcasted_iota(jnp.int32, (BLOCK, BLOCK), 1), 1.0, 0.0
    ).astype(BF16)

    def stacked(v):
        return jnp.concatenate([jnp.where(low64, v, 0.0), jnp.where(low64, 0.0, v)], axis=0)

    def pairs(a, q, b, k):
        left = jnp.concatenate([stacked(a), stacked(q)], axis=0)
        out = mm_nt_wide(left, jnp.concatenate([b, k, k, b], axis=0))
        head1 = lane >= HEAD
        first, second = out[:, :LANES], out[:, LANES:]
        pick = lambda f, g: jnp.where(head1, g, f)
        return (
            pick(first[:128], second[:128]), pick(second[:128], first[:128]),
            pick(first[128:], second[128:]), pick(second[128:], first[128:]),
        )

    def one_block(n):
        rows = pl.ds(pl.multiple_of(n * BLOCK, BLOCK), BLOCK)
        ld = LD[rows, :]
        lh, ll = halves(ld)
        lll = (ld - lh.astype(F32) - ll.astype(F32)).astype(BF16)
        L = dot(tri, lh) + dot(tri, ll) + dot(tri, lll)
        Lx = L - ld
        a, b, k = AD[rows, :], BD[rows, :], KW[rows, :]
        q = proj_ref[rows, 3 * LANES : 4 * LANES].astype(F32)
        v = proj_ref[rows, 5 * LANES : 6 * LANES].astype(F32)
        mid = jnp.where(row64 < 32, L[15:16, :], L[47:48, :])
        edge, end = L[31:32, :], L[63:64, :]
        back = jnp.exp(mid - L)
        near = pairs(a * jnp.exp(Lx - mid), q * jnp.exp(L - mid), b * back, k * back)
        back = jnp.exp(jnp.minimum(edge - L, 0.0))
        far = pairs(
            a * jnp.exp(jnp.minimum(Lx - edge, 0.0)), q * jnp.exp(jnp.minimum(L - edge, 0.0)), b * back, k * back
        )
        M, N, QB, QK = (
            jnp.where(mask, jnp.where(same32, f, g), 0.0) for mask, f, g in zip((strict, strict, causal, causal), near, far)
        )
        As, Vs = stacked(a * jnp.exp(Lx)), stacked(v)
        inv = eye + jnp.where(offs[1], M, 0.0)
        for w in (2, 4, 8, 16, 32):
            inv = inv + mm(mm(inv, jnp.where(offs[w], M, 0.0)), inv)
        both = mm_wide(inv, jnp.concatenate([As, mm(N, Vs)], axis=1))
        qboth = mm_wide(QB, both)
        qm = stacked(q * jnp.exp(L)) + qboth[:, :LANES]
        lo = qboth[:, LANES:] + mm(QK, Vs)
        ahead = jnp.exp(end - L)
        smT, leT = both[:, :LANES].T, both[:, LANES:].T
        gl = mm(jnp.concatenate([smT, leT], axis=0), stacked(b * ahead))
        G = gl[:128] + jnp.where(row == lane, jnp.exp(end), 0.0)
        H = gl[128:] + mm(Vs.T, stacked(k * ahead))
        GC[n, 0] = G
        GC[n, 1] = H
        QM[n] = qm
        LO[n] = lo[:BLOCK] + lo[BLOCK:]

    @pl.loop(0, 4)
    def _(i):
        for u in range(4):
            one_block(i * 4 + u)

    X[0:128, :] = eye
    X[128:256, :] = jnp.zeros((128, LANES), F32)

    @pl.loop(0, 4)
    def _(i):
        for u in range(4):
            n = i * 4 + u
            rows = pl.ds(pl.multiple_of(n * BLOCK, BLOCK), BLOCK)
            before = X[...]
            out = mm_nt_wide(QM[n], before)
            qp_ref[rows, :] = out[:BLOCK, :LANES] + out[BLOCK:, :LANES]
            loc_ref[rows, :] = out[:BLOCK, LANES:] + out[BLOCK:, LANES:] + LO[n]
            after = mm(before, GC[n, 0])
            X[0:128, :] = after[:128]
            X[128:256, :] = after[128:] + GC[n, 1]

    gh_ref[0:64, :] = (X[0:64, :] + X[64:128, :]).astype(BF16)
    gh_ref[64:128, :] = (X[128:192, :] + X[192:256, :]).astype(BF16)


def block_terms(proj, low, shift, up_d, up_r, par):
    vmem = pl.BlockSpec(memory_space=pltpu.VMEM)

    def kernel(*refs):
        block_kernel(None, *refs)

    return pl.pallas_call(
        kernel,
        name="block_terms",
        out_shape=(
            jax.ShapeDtypeStruct((1024, LANES), F32),
            jax.ShapeDtypeStruct((1024, LANES), F32),
            jax.ShapeDtypeStruct((128, LANES), BF16),
        ),
        in_specs=[vmem] * 6,
        out_specs=(vmem,) * 3,
        scratch_shapes=[
            pltpu.VMEM((1024, LANES), F32),
            pltpu.VMEM((1024, LANES), F32),
            pltpu.VMEM((1024, LANES), F32),
            pltpu.VMEM((1024, LANES), F32),
            pltpu.VMEM((16, 2, 128, LANES), F32),
            pltpu.VMEM((16, 128, LANES), F32),
            pltpu.VMEM((16, BLOCK, LANES), F32),
            pltpu.VMEM((256, LANES), F32),
        ],
        compiler_params=pltpu.CompilerParams(vmem_limit_bytes=48 << 20),
        cost_estimate=pl.CostEstimate(flops=4_000_000_000, bytes_accessed=4_000_000, transcendentals=2_000_000),
    )(proj, low, shift, up_d, up_r, par)


def finish_kernel(
    proj_ref, qp_ref, loc_ref, gh_ref, wout_ref, par_ref,
    out_ref,
    CH, HALO, S, Z, SB, RB, OB, S1, S2, R1, R2, S3, S4, R3, R4,
    g_send, g_recv, h_send, h_recv, b_send, b_recv, y_send, y_recv,
):
    z, y, x, c = here()

    def at(dz=0, dy=0, dc=0):
        return (lax.rem(z + dz, NZ), lax.rem(y + dy, NY), x, lax.rem(c + dc, 2))

    entered = enter([at(dz=d) for d in range(1, NZ)] + [at(dy=1), at(dy=3), at(dc=1)])
    mine = pl.ds(pl.multiple_of(y * LANES, LANES), LANES)
    entered()

    def chain_copy(d):
        return remote(gh_ref, CH.at[z], g_send.at[d], g_recv.at[z], at(dz=d))

    def halo_copy(k):
        return remote(proj_ref.at[1008:1024, k * LANES : k * LANES + LANES], HALO.at[k - 1], h_send.at[k - 1], h_recv.at[k - 1], at(dz=1))

    for d in range(1, NZ):

        @pl.when(z + d < NZ)
        def _():
            if d == 1:
                halo_copy(1).start()
                halo_copy(2).start()
            chain_copy(d).start()

    HALO_ZERO = jnp.zeros((16, LANES), BF16)

    @pl.when(z > 0)
    def _():
        halo_copy(1).wait_recv()
        halo_copy(2).wait_recv()

    @pl.when(z == 0)
    def _():
        HALO[0] = HALO_ZERO
        HALO[1] = HALO_ZERO

    tap0, tap1, tap2 = (par_ref[5 + k : 6 + k, mine] for k in range(3))
    before = HALO[0].astype(F32) * HALO[1].astype(F32)
    product = proj_ref[:, LANES : 2 * LANES].astype(F32) * proj_ref[:, 2 * LANES : 3 * LANES].astype(F32)
    whole = jnp.concatenate([before[8:16], product], axis=0)
    filtered = tap0 * whole[6:1030] + tap1 * whole[7:1031] + tap2 * product
    Z[:, 0:LANES] = (proj_ref[:, 0:LANES].astype(F32) * filtered).astype(BF16)

    low64 = lax.broadcasted_iota(jnp.int32, (HEAD, LANES), 1) < HEAD

    def stacked(v):
        zero = jnp.zeros_like(v)
        return jnp.concatenate([jnp.where(low64, v, zero), jnp.where(low64, zero, v)], axis=0)

    S[...] = jnp.zeros((HEAD, LANES), F32)
    for k in range(NZ - 1):

        @pl.when(z > k)
        def _():
            remote(gh_ref, CH.at[k], g_send.at[1], g_recv.at[k], at(dz=1)).wait_recv()
            high, low = halves(S[...])
            g = stacked(CH[k, 0:64, :])
            S[...] = dot(high, g) + dot(low, g) + CH[k, 64:128, :].astype(F32)

    lane = lax.broadcasted_iota(jnp.int32, (128, LANES), 1)
    row = lax.broadcasted_iota(jnp.int32, (128, LANES), 0)
    mean_of = jnp.where((row // HEAD) == (lane // HEAD), 1.0 / HEAD, 0.0).astype(BF16)
    start = stacked(S[...])
    start_h, start_l = halves(start)
    gain = par_ref[4:5, mine]

    @pl.loop(0, 4)
    def _(i):
        rows = pl.ds(pl.multiple_of(i * 256, 256), 256)
        qh, ql = halves(qp_ref[rows, :])
        readout = loc_ref[rows, :] + dot_nt(qh, start_h) + dot_nt(ql, start_h) + dot_nt(qh, start_l)
        centered = readout - head_sum(readout, mean_of)
        variance = head_sum(centered * centered, mean_of)
        Z[rows, LANES : 2 * LANES] = (centered * lax.rsqrt(variance + group_eps) * gain).astype(BF16)

    rel = (2, 1, 3, 0)
    other = at(dc=1)

    def to_other(k):
        return remote(SB.at[k], RB.at[k], b_send.at[k], b_recv.at[k], other)

    def part(k, core):
        rows = pl.ds(pl.multiple_of((lax.rem(y + rel[k], NY) * 2 + core) * 128, 128), 128)
        return dot_nt(Z[rows, :], wout_ref[...])

    for k in range(4):
        SB[k] = part(k, 1 - c).astype(BF16)
        to_other(k).start()
        OB[k] = part(k, c)

    def total(k, lo, hi):
        return OB[k, lo:hi, :] + RB[k, lo:hi, :].astype(F32)

    up, down = at(dy=1), at(dy=3)
    c1 = remote(S1, R1, y_send.at[0], y_recv.at[0], up)
    c2 = remote(S2, R2, y_send.at[1], y_recv.at[1], down)
    c3b = remote(S3.at[64:128], R3.at[64:128], y_send.at[2], y_recv.at[2], up)
    c4a = remote(S4.at[0:64], R4.at[0:64], y_send.at[3], y_recv.at[3], down)
    c3a = remote(S3.at[0:64], R3.at[0:64], y_send.at[4], y_recv.at[4], up)
    c4b = remote(S4.at[64:128], R4.at[64:128], y_send.at[5], y_recv.at[5], down)
    to_other(0).wait_recv()
    S1[...] = total(0, 0, 64).astype(BF16)
    S2[...] = total(0, 64, 128).astype(BF16)
    to_other(1).wait_recv()
    c1.start()
    c2.start()
    S3[64:128, :] = total(1, 64, 128).astype(BF16)
    to_other(2).wait_recv()
    S4[0:64, :] = total(2, 0, 64).astype(BF16)
    c3b.start()
    to_other(3).wait_recv()
    c4a.start()
    OB[3] = OB[3] + RB[3].astype(F32)
    c1.wait_recv()
    S3[0:64, :] = (total(1, 0, 64) + R1[...].astype(F32)).astype(BF16)
    c2.wait_recv()
    c3a.start()
    S4[64:128, :] = (total(2, 64, 128) + R2[...].astype(F32)).astype(BF16)
    c3b.wait_recv()
    c4b.start()
    c4a.wait_recv()
    c3a.wait_recv()
    c4b.wait_recv()
    out_ref[...] = (OB[3] + R3[...].astype(F32) + R4[...].astype(F32)).astype(BF16)
    for copy in (c1, c2, c3b, c4a, c3a, c4b):
        copy.wait_send()
    for k in range(4):
        to_other(k).wait_send()
    for d in range(1, NZ):

        @pl.when(z + d < NZ)
        def _():
            if d == 1:
                halo_copy(1).wait_send()
                halo_copy(2).wait_send()
            chain_copy(d).wait_send()


def finish(proj, qp, loc, gh, wout, par):
    vmem = pl.BlockSpec(memory_space=pltpu.VMEM)
    dma = pltpu.SemaphoreType.DMA
    block = lambda n: pltpu.VMEM((n, 2048), BF16)
    return pl.pallas_call(
        finish_kernel,
        name="finish",
        out_shape=jax.ShapeDtypeStruct((128, 2048), BF16),
        in_specs=[vmem] * 6,
        out_specs=vmem,
        scratch_shapes=[
            pltpu.VMEM((NZ, 128, LANES), BF16),
            pltpu.VMEM((2, 16, LANES), BF16),
            pltpu.VMEM((HEAD, LANES), F32),
            pltpu.VMEM((1024, 2 * LANES), BF16),
            pltpu.VMEM((4, 128, 2048), BF16),
            pltpu.VMEM((4, 128, 2048), BF16),
            pltpu.VMEM((4, 128, 2048), F32),
            block(64), block(64), block(64), block(64), block(128), block(128), block(128), block(128),
            dma((NZ,)), dma((NZ,)), dma((2,)), dma((2,)), dma((4,)), dma((4,)), dma((6,)), dma((6,)),
        ],
        compiler_params=pltpu.CompilerParams(collective_id=2, has_side_effects=True, vmem_limit_bytes=48 << 20),
        cost_estimate=pl.CostEstimate(flops=1_500_000_000, bytes_accessed=8_000_000, transcendentals=0),
    )(proj, qp, loc, gh, wout, par)


def body(
    tokens, norm_gain, w_conv_gate, w_conv_in, w_conv_value, conv_taps, w_receptance, w_key, w_value, w_decay_down,
    w_decay_up, decay_base, decay_shift, w_rate_down, w_rate_up, rate_base, key_scale, key_mix, group_gain,
    w_out_conv, w_out_state,
):
    first = lax.axis_index("tp") == 0
    low = jnp.where(first, w_decay_down, w_rate_down)
    pieces = [w.reshape(64, NY, LANES) for w in (w_conv_gate, w_conv_in, w_conv_value, w_receptance, w_key, w_value)]
    pieces.append(jnp.broadcast_to(low[:, None, :], (64, NY, LANES)))
    pieces += [w.T.reshape(64, NY, LANES) for w in (w_out_conv, w_out_state)]
    wp = jnp.concatenate(pieces, axis=2).transpose(1, 0, 2)
    par = jnp.concatenate(
        [jnp.stack([decay_base, rate_base, key_scale, key_mix, group_gain]), conv_taps], axis=0
    )
    proj, low, shift, wout = gather_and_project(tokens[0], norm_gain[None], wp, decay_shift[0])
    qp, loc, gh = block_terms(proj, low, shift, w_decay_up, w_rate_up, par)
    return finish(proj, qp, loc, gh, wout, par)[None]


def solution(mesh):
    split = Mesh(mesh.devices.reshape(NZ, NY, mesh.shape["fs"], mesh.shape["tp"]), AXES)
    placed = (
        P("fs", SP_TP, None), P(), P(SP, "tp"), P(SP, "tp"), P(SP, "tp"), P(None, "tp"), P(SP, "tp"), P(SP, "tp"),
        P(SP, "tp"), P(SP, None), P(None, "tp"), P("tp"), P("fs", SP, "tp"), P(SP, None), P(None, "tp"), P("tp"),
        P("tp"), P("tp"), P("tp"), P("tp", SP), P("tp", SP),
    )
    return jax.shard_map(
        body, mesh=split, in_specs=placed, out_specs=P("fs", SP_TP, None), check_vma=False
    )
```

```python
import jax
import jax.numpy as jnp
from jax import lax
from jax.experimental import pallas as pl
from jax.experimental.pallas import tpu as pltpu
from jax.sharding import Mesh
from jax.sharding import PartitionSpec as P

MESH = pl.DeviceIdType.MESH
AXES = ("sp_0", "sp_1", "fs", "tp")
SP = ("sp_0", "sp_1")
SP_TP = ("sp_0", "sp_1", "tp")
NZ, NY, NX = 8, 4, 4
HEAD = 64
LANES = 128
BLOCK = 64
COLS_IN = 7 * LANES
COLS = 9 * LANES
F32, BF16 = jnp.float32, jnp.bfloat16
norm_eps = 1e-06
group_eps = 0.00064


def here():
    return tuple(lax.axis_index(a) for a in AXES)


def enter(peers):
    barrier = pltpu.get_barrier_semaphore()
    for peer in peers:
        pl.semaphore_signal(barrier, inc=1, device_id=peer, device_id_type=MESH)
    return lambda: pl.semaphore_wait(barrier, len(peers))


def remote(src, dst, send_sem, recv_sem, peer):
    return pltpu.make_async_remote_copy(
        src_ref=src, dst_ref=dst, send_sem=send_sem, recv_sem=recv_sem, device_id=peer, device_id_type=MESH
    )


def gather_kernel(
    tok_ref, gain_ref, wp_ref, shift_ref,
    proj_ref, low_ref, shift_out, wout_ref,
    T, W, DS, LOW,
    w_send, w_recv, a_send, a_recv, s_send, s_recv, t_send, t_recv, c_send, c_recv, l_send, l_recv,
):
    z, y, x, c = here()

    def at(dz=0, dy=0, dx=0, dc=0):
        return (lax.rem(z + dz, NZ), lax.rem(y + dy, NY), lax.rem(x + dx, NX), lax.rem(c + dc, 2))

    peers = [at(dz=1), at(dz=7), at(dx=1), at(dx=3), at(dy=1), at(dy=2), at(dy=3), at(dc=1)]
    entered = enter(peers)
    x16 = pl.multiple_of(x * 16, 16)
    lane_of = lambda yy: pl.ds(pl.multiple_of(yy * LANES, LANES), LANES)
    W[z, y, x] = wp_ref[y, pl.ds(x16, 16), :]
    DS[y] = shift_ref[:, lane_of(y)]
    gain = gain_ref[...]

    @pl.loop(0, 4)
    def _(i):
        rows = pl.ds(pl.multiple_of(i * 32, 32), 32)
        values = tok_ref[rows, :].astype(F32)
        scaled = values * lax.rsqrt(jnp.mean(values * values, axis=-1, keepdims=True) + norm_eps)
        T[y, c, rows, :] = (scaled * gain).astype(BF16)

    entered()
    waits = []

    def go(copy):
        copy.start()
        waits.append(copy)
        return copy

    arrive_a = []
    for d in (1, 3, 2):
        to = lax.rem(y + d, NY)
        arrive_a.append(go(remote(wp_ref.at[to, pl.ds(x16, 16), :], W.at[z, y, x], a_send.at[d - 1], a_recv.at[d - 1], at(dy=d))))
    def token_unit(dy, half):
        return T.at[lax.rem(y + NY - dy, NY), c, pl.ds(half * 64, 64), :]

    def token_send(dy, half, to_dy, via):
        k = to_dy * 2 + half
        return go(remote(token_unit(dy, half), token_unit(dy, half), t_send.at[k], t_recv.at[k], at(dy=via)))

    t10 = token_send(0, 0, 1, 1)
    t31 = token_send(0, 1, 3, 3)
    t11 = token_send(0, 1, 1, 1)
    t30 = token_send(0, 0, 3, 3)
    other = at(dc=1)

    def across(dy):
        unit = T.at[lax.rem(y + NY - dy, NY), c]
        return go(remote(unit, unit, c_send.at[dy], c_recv.at[dy], other))

    crossed = [across(0)]
    for d in (1, 3, 2):
        to = lax.rem(y + d, NY)
        go(remote(shift_ref.at[:, lane_of(to)], DS.at[y], s_send.at[d - 1], s_recv.at[d - 1], at(dy=d)))

    def unit(h, dz, dx):
        return W.at[lax.rem(z + NZ - dz, NZ), pl.ds(2 * h, 2), lax.rem(x + NX - dx, NX)]

    copies = {}

    def send(h, dz, dx, step_z, step_x):
        nz, nx = (dz + step_z) % NZ, (dx + step_x) % NX
        copies[h, nz, nx] = go(
            remote(unit(h, dz, dx), unit(h, dz, dx), w_send.at[h, nz, nx], w_recv.at[h, nz, nx], at(dz=step_z % NZ, dx=step_x % NX))
        )

    def forward(h, dz, dx):
        if h == 0:
            if dx == 0:
                if dz in (0, 1, 2, 3):
                    send(0, dz, 0, 1, 0)
                if dz in (0, 7, 6):
                    send(0, dz, 0, -1, 0)
                send(0, dz, 0, 0, 1)
                send(0, dz, 0, 0, -1)
            elif dx == 1 and dz % 2 == 0:
                send(0, dz, 1, 0, 1)
            elif dx == 3 and dz % 2 == 1:
                send(0, dz, 3, 0, -1)
        else:
            if dz == 0:
                if dx in (0, 1):
                    send(1, 0, dx, 0, 1)
                if dx == 0:
                    send(1, 0, dx, 0, -1)
                send(1, 0, dx, 1, 0)
                send(1, 0, dx, -1, 0)
            elif dz in (1, 2) or (dz == 3 and dx % 2 == 0):
                send(1, dz, dx, 1, 0)
            elif dz in (7, 6) or (dz == 5 and dx % 2 == 1):
                send(1, dz, dx, -1, 0)

    def hops(h, dz, dx):
        return min(dz, NZ - dz) + min(dx, NX - dx)

    for copy in arrive_a:
        copy.wait_recv()
    order = sorted(
        ((h, dz, dx) for h in range(2) for dz in range(NZ) for dx in range(NX)),
        key=lambda u: (hops(*u), u[0], min(u[2], NX - u[2]), u[1]),
    )
    token_at = 12
    for k, u in enumerate(order):
        if k >= 2:
            copies[u].wait_recv()
        forward(*u)
        if k == token_at:
            t10.wait_recv()
            t20 = token_send(1, 0, 2, 1)
            t31.wait_recv()
            t21 = token_send(3, 1, 2, 3)
        if k == token_at + 16:
            t11.wait_recv()
            t30.wait_recv()
            crossed += [across(1), across(3)]
    t20.wait_recv()
    t21.wait_recv()
    crossed.append(across(2))
    for copy in crossed:
        copy.wait_recv()

    def project(first, count):
        rows = T[...].reshape(1024, 2048)
        w = W[:, :, :, :, first * LANES : (first + count) * LANES].reshape(2048, count * LANES)
        return jnp.dot(rows, w, preferred_element_type=F32).astype(BF16)

    LOW[c] = project(6, 1)
    low_copy = remote(LOW.at[c], LOW.at[c], l_send.at[0], l_recv.at[0], other)
    low_copy.start()
    for n in (0, 2, 4):
        proj_ref[:, n * LANES : (n + 2) * LANES] = project(n, 2)

    wout_ref[...] = W[:, :, :, :, 7 * LANES :].reshape(2048, 256)
    for d in (1, 2, 3):
        to = lax.rem(y + d, NY)
        remote(shift_ref.at[:, lane_of(to)], DS.at[y], s_send.at[d - 1], s_recv.at[d - 1], at(dy=d)).wait_recv()
    shift_out[...] = DS[...].reshape(1024, LANES)
    low_copy.wait_recv()
    low_ref[...] = LOW[...]
    low_copy.wait_send()
    for copy in waits:
        copy.wait_send()


def gather_and_project(tokens, gain, wp, shift):
    vmem = pl.BlockSpec(memory_space=pltpu.VMEM)
    dma = pltpu.SemaphoreType.DMA
    return pl.pallas_call(
        gather_kernel,
        name="gather_project",
        out_shape=(
            jax.ShapeDtypeStruct((1024, 6 * LANES), BF16),
            jax.ShapeDtypeStruct((2, 1024, LANES), BF16),
            jax.ShapeDtypeStruct((1024, LANES), F32),
            jax.ShapeDtypeStruct((2048, 2 * LANES), BF16),
        ),
        in_specs=[vmem] * 4,
        out_specs=(vmem,) * 4,
        scratch_shapes=[
            pltpu.VMEM((NY, 2, 128, 2048), BF16),
            pltpu.VMEM((NZ, NY, NX, 16, COLS), BF16),
            pltpu.VMEM((NY, 256, LANES), F32),
            pltpu.VMEM((2, 1024, LANES), BF16),
            dma((2, NZ, NX)), dma((2, NZ, NX)), dma((3,)), dma((3,)), dma((3,)), dma((3,)),
            dma((8,)), dma((8,)), dma((4,)), dma((4,)), dma((1,)), dma((1,)),
        ],
        compiler_params=pltpu.CompilerParams(collective_id=1, has_side_effects=True, vmem_limit_bytes=48 << 20),
        cost_estimate=pl.CostEstimate(flops=4_000_000_000, bytes_accessed=16_000_000, transcendentals=0),
    )(tokens, gain, wp, shift)


def halves(a):
    high = a.astype(BF16)
    return high, (a - high.astype(F32)).astype(BF16)


def dot(a, b):
    return jnp.dot(a, b, preferred_element_type=F32)


def dot_nt(a, b):
    return lax.dot_general(a, b, (((1,), (1,)), ((), ())), preferred_element_type=F32)


def mm(a, b):
    ah, al = halves(a)
    bh, bl = halves(b)
    both = jnp.concatenate([bh, bl], axis=1)
    out = dot(jnp.concatenate([ah, al], axis=1), jnp.concatenate([both, both], axis=0))
    return out[:, :LANES] + out[:, LANES:]


def mm1(a, b):
    return dot(a.astype(BF16), b.astype(BF16))


def nt1(a, b):
    return dot_nt(a.astype(BF16), b.astype(BF16))


def head_sum(values, ones):
    high, low = halves(values)
    return dot(high, ones) + dot(low, ones)


def block_kernel(
    y_param, proj_ref, low_ref, shift_ref, up_d_ref, up_r_ref, par_ref,
    qp_ref, loc_ref, gh_ref,
    LD, AD, BD, KW, GC, QM, LO, X,
):
    y = lax.axis_index("sp_1")
    mine = pl.ds(pl.multiple_of(y * LANES, LANES), LANES)
    lane = lax.broadcasted_iota(jnp.int32, (128, LANES), 1)
    row = lax.broadcasted_iota(jnp.int32, (128, LANES), 0)
    same_head = (row // HEAD) == (lane // HEAD)
    ones = jnp.where(same_head, 1.0, 0.0).astype(BF16)
    up_d, up_r = up_d_ref[:, mine], up_r_ref[:, mine]
    decay_base, rate_base = par_ref[0:1, mine], par_ref[1:2, mine]
    key_scale, key_mix = par_ref[2:3, mine], par_ref[3:4, mine]

    @pl.loop(0, 4)
    def _(i):
        rows = pl.ds(pl.multiple_of(i * 256, 256), 256)
        act = jnp.tanh(low_ref[0, rows, :].astype(F32)).astype(BF16)
        pre = decay_base + dot(act, up_d)
        LD[rows, :] = shift_ref[rows, :] - jax.nn.sigmoid(pre) * 0.6065306597126334
        rate = jax.nn.sigmoid(rate_base + dot(low_ref[1, rows, :], up_r))
        key = proj_ref[rows, 4 * LANES : 5 * LANES].astype(F32)
        scaled = key * key_scale
        erase = scaled * lax.rsqrt(head_sum(scaled * scaled, ones) + norm_eps)
        AD[rows, :] = -erase
        BD[rows, :] = erase * rate
        KW[rows, :] = key * (1.0 + (rate - 1.0) * key_mix)

    t, s = row % HEAD, lane % HEAD
    strict = same_head & (t > s)
    causal = same_head & (t >= s)
    same32 = (t // 32) == (s // 32)
    eye = jnp.where(row == lane, 1.0, 0.0)
    offs = {
        b: same_head & ((t // (2 * b)) == (s // (2 * b))) & ((t // b) % 2 == 1) & ((s // b) % 2 == 0) for b in (1, 2, 4, 8, 16, 32)
    }
    low64 = lax.broadcasted_iota(jnp.int32, (BLOCK, LANES), 1) < HEAD
    row64 = lax.broadcasted_iota(jnp.int32, (BLOCK, LANES), 0)
    tri = jnp.where(
        lax.broadcasted_iota(jnp.int32, (BLOCK, BLOCK), 0) >= lax.broadcasted_iota(jnp.int32, (BLOCK, BLOCK), 1), 1.0, 0.0
    ).astype(BF16)

    def stacked(v):
        return jnp.concatenate([jnp.where(low64, v, 0.0), jnp.where(low64, 0.0, v)], axis=0)

    def pairs(a, q, b, k):
        left = jnp.concatenate([stacked(a), stacked(q)], axis=0)
        out = nt1(left, jnp.concatenate([b, k, k, b], axis=0))
        head1 = lane >= HEAD
        first, second = out[:, :LANES], out[:, LANES:]
        pick = lambda f, g: jnp.where(head1, g, f)
        return (
            pick(first[:128], second[:128]), pick(second[:128], first[:128]),
            pick(first[128:], second[128:]), pick(second[128:], first[128:]),
        )

    def one_block(n):
        rows = pl.ds(n * BLOCK, BLOCK)
        ld = LD[rows, :]
        lh, ll = halves(ld)
        lll = (ld - lh.astype(F32) - ll.astype(F32)).astype(BF16)
        L = dot(tri, lh) + dot(tri, ll) + dot(tri, lll)
        Lx = L - ld
        a, b, k = AD[rows, :], BD[rows, :], KW[rows, :]
        q = proj_ref[rows, 3 * LANES : 4 * LANES].astype(F32)
        v = proj_ref[rows, 5 * LANES : 6 * LANES].astype(F32)
        mid = jnp.where(row64 < 32, L[15:16, :], L[47:48, :])
        edge, end = L[31:32, :], L[63:64, :]
        back = jnp.exp(mid - L)
        near = pairs(a * jnp.exp(Lx - mid), q * jnp.exp(L - mid), b * back, k * back)
        yield
        back = jnp.exp(jnp.minimum(edge - L, 0.0))
        far = pairs(
            a * jnp.exp(jnp.minimum(Lx - edge, 0.0)), q * jnp.exp(jnp.minimum(L - edge, 0.0)), b * back, k * back
        )
        yield
        M, N, QB, QK = (
            jnp.where(mask, jnp.where(same32, f, g), 0.0) for mask, f, g in zip((strict, strict, causal, causal), near, far)
        )
        As, Vs = stacked(a * jnp.exp(Lx)), stacked(v)
        NV = mm1(N, Vs)
        yield
        lo = mm1(QK, Vs)
        yield
        inv = eye + jnp.where(offs[1], M, 0.0)
        for w in (2, 4, 8, 16, 32):
            part = mm(inv, jnp.where(offs[w], M, 0.0))
            yield
            inv = inv + mm(part, inv)
            yield
        both = mm1(inv, jnp.concatenate([As, NV], axis=1))
        yield
        qboth = mm1(QB, both)
        yield
        qm = stacked(q * jnp.exp(L)) + qboth[:, :LANES]
        lo = qboth[:, LANES:] + lo
        QM[n] = qm
        LO[n] = lo[:BLOCK] + lo[BLOCK:]
        ahead = jnp.exp(end - L)
        smT, leT = both[:, :LANES].T, both[:, LANES:].T
        gl = mm1(jnp.concatenate([smT, leT], axis=0), stacked(b * ahead))
        yield
        G = gl[:128] + jnp.where(row == lane, jnp.exp(end), 0.0)
        H = gl[128:] + mm1(Vs.T, stacked(k * ahead))
        GC[n, 0] = G
        GC[n, 1] = H

    def in_step(blocks):
        blocks = list(blocks)
        while blocks:
            blocks = [b for b in blocks if next(b, True) is None]

    in_step(one_block(u) for u in range(16))

    X[0:128, :] = eye
    X[128:256, :] = jnp.zeros((128, LANES), F32)

    @pl.loop(0, 4)
    def _(i):
        for u in range(4):
            n = i * 4 + u
            rows = pl.ds(pl.multiple_of(n * BLOCK, BLOCK), BLOCK)
            before = X[...]
            out = nt1(QM[n], before)
            qp_ref[rows, :] = out[:BLOCK, :LANES] + out[BLOCK:, :LANES]
            loc_ref[rows, :] = out[:BLOCK, LANES:] + out[BLOCK:, LANES:] + LO[n]
            after = mm(before, GC[n, 0])
            X[0:128, :] = after[:128]
            X[128:256, :] = after[128:] + GC[n, 1]

    gh_ref[0:64, :] = (X[0:64, :] + X[64:128, :]).astype(BF16)
    gh_ref[64:128, :] = (X[128:192, :] + X[192:256, :]).astype(BF16)


def block_terms(proj, low, shift, up_d, up_r, par):
    vmem = pl.BlockSpec(memory_space=pltpu.VMEM)

    def kernel(*refs):
        block_kernel(None, *refs)

    return pl.pallas_call(
        kernel,
        name="block_terms",
        out_shape=(
            jax.ShapeDtypeStruct((1024, LANES), F32),
            jax.ShapeDtypeStruct((1024, LANES), F32),
            jax.ShapeDtypeStruct((128, LANES), BF16),
        ),
        in_specs=[vmem] * 6,
        out_specs=(vmem,) * 3,
        scratch_shapes=[
            pltpu.VMEM((1024, LANES), F32),
            pltpu.VMEM((1024, LANES), F32),
            pltpu.VMEM((1024, LANES), F32),
            pltpu.VMEM((1024, LANES), F32),
            pltpu.VMEM((16, 2, 128, LANES), F32),
            pltpu.VMEM((16, 128, LANES), F32),
            pltpu.VMEM((16, BLOCK, LANES), F32),
            pltpu.VMEM((256, LANES), F32),
        ],
        compiler_params=pltpu.CompilerParams(vmem_limit_bytes=48 << 20),
        cost_estimate=pl.CostEstimate(flops=4_000_000_000, bytes_accessed=4_000_000, transcendentals=2_000_000),
    )(proj, low, shift, up_d, up_r, par)


def finish_kernel(
    proj_ref, qp_ref, loc_ref, gh_ref, wout_ref, par_ref,
    out_ref,
    CH, HALO, S, Z, SB, RB, OB, S1, S2, R1, R2, S3, S4, R3, R4,
    g_send, g_recv, h_send, h_recv, b_send, b_recv, y_send, y_recv,
):
    z, y, x, c = here()

    def at(dz=0, dy=0, dc=0):
        return (lax.rem(z + dz, NZ), lax.rem(y + dy, NY), x, lax.rem(c + dc, 2))

    entered = enter([at(dz=d) for d in range(1, NZ)] + [at(dy=1), at(dy=3), at(dc=1)])
    mine = pl.ds(pl.multiple_of(y * LANES, LANES), LANES)
    entered()

    def chain_copy(d):
        return remote(gh_ref, CH.at[z], g_send.at[d], g_recv.at[z], at(dz=d))

    def halo_copy(k):
        return remote(proj_ref.at[1008:1024, k * LANES : k * LANES + LANES], HALO.at[k - 1], h_send.at[k - 1], h_recv.at[k - 1], at(dz=1))

    for d in range(1, NZ):

        @pl.when(z + d < NZ)
        def _():
            if d == 1:
                halo_copy(1).start()
                halo_copy(2).start()
            chain_copy(d).start()

    HALO_ZERO = jnp.zeros((16, LANES), BF16)

    @pl.when(z > 0)
    def _():
        halo_copy(1).wait_recv()
        halo_copy(2).wait_recv()

    @pl.when(z == 0)
    def _():
        HALO[0] = HALO_ZERO
        HALO[1] = HALO_ZERO

    tap0, tap1, tap2 = (par_ref[5 + k : 6 + k, mine] for k in range(3))
    before = HALO[0].astype(F32) * HALO[1].astype(F32)
    product = proj_ref[:, LANES : 2 * LANES].astype(F32) * proj_ref[:, 2 * LANES : 3 * LANES].astype(F32)
    whole = jnp.concatenate([before[8:16], product], axis=0)
    filtered = tap0 * whole[6:1030] + tap1 * whole[7:1031] + tap2 * product
    Z[:, 0:LANES] = (proj_ref[:, 0:LANES].astype(F32) * filtered).astype(BF16)

    low64 = lax.broadcasted_iota(jnp.int32, (HEAD, LANES), 1) < HEAD

    def stacked(v):
        zero = jnp.zeros_like(v)
        return jnp.concatenate([jnp.where(low64, v, zero), jnp.where(low64, zero, v)], axis=0)

    S[...] = jnp.zeros((HEAD, LANES), F32)
    for k in range(NZ - 1):

        @pl.when(z > k)
        def _():
            remote(gh_ref, CH.at[k], g_send.at[1], g_recv.at[k], at(dz=1)).wait_recv()
            high, low = halves(S[...])
            g = stacked(CH[k, 0:64, :])
            S[...] = dot(high, g) + dot(low, g) + CH[k, 64:128, :].astype(F32)

    lane = lax.broadcasted_iota(jnp.int32, (128, LANES), 1)
    row = lax.broadcasted_iota(jnp.int32, (128, LANES), 0)
    mean_of = jnp.where((row // HEAD) == (lane // HEAD), 1.0 / HEAD, 0.0).astype(BF16)
    start = stacked(S[...])
    start_h, start_l = halves(start)
    gain = par_ref[4:5, mine]

    @pl.loop(0, 4)
    def _(i):
        rows = pl.ds(pl.multiple_of(i * 256, 256), 256)
        qh, ql = halves(qp_ref[rows, :])
        readout = loc_ref[rows, :] + dot_nt(qh, start_h) + dot_nt(ql, start_h) + dot_nt(qh, start_l)
        centered = readout - head_sum(readout, mean_of)
        variance = head_sum(centered * centered, mean_of)
        Z[rows, LANES : 2 * LANES] = (centered * lax.rsqrt(variance + group_eps) * gain).astype(BF16)

    rel = (2, 1, 3, 0)
    other = at(dc=1)

    def to_other(k):
        return remote(SB.at[k], RB.at[k], b_send.at[k], b_recv.at[k], other)

    def part(k, core):
        rows = pl.ds(pl.multiple_of((lax.rem(y + rel[k], NY) * 2 + core) * 128, 128), 128)
        return dot_nt(Z[rows, :], wout_ref[...])

    for k in range(4):
        SB[k] = part(k, 1 - c).astype(BF16)
        to_other(k).start()
        OB[k] = part(k, c)

    def total(k, lo, hi):
        return OB[k, lo:hi, :] + RB[k, lo:hi, :].astype(F32)

    up, down = at(dy=1), at(dy=3)
    c1 = remote(S1, R1, y_send.at[0], y_recv.at[0], up)
    c2 = remote(S2, R2, y_send.at[1], y_recv.at[1], down)
    c3b = remote(S3.at[64:128], R3.at[64:128], y_send.at[2], y_recv.at[2], up)
    c4a = remote(S4.at[0:64], R4.at[0:64], y_send.at[3], y_recv.at[3], down)
    c3a = remote(S3.at[0:64], R3.at[0:64], y_send.at[4], y_recv.at[4], up)
    c4b = remote(S4.at[64:128], R4.at[64:128], y_send.at[5], y_recv.at[5], down)
    to_other(0).wait_recv()
    S1[...] = total(0, 0, 64).astype(BF16)
    S2[...] = total(0, 64, 128).astype(BF16)
    to_other(1).wait_recv()
    c1.start()
    c2.start()
    S3[64:128, :] = total(1, 64, 128).astype(BF16)
    to_other(2).wait_recv()
    S4[0:64, :] = total(2, 0, 64).astype(BF16)
    c3b.start()
    to_other(3).wait_recv()
    c4a.start()
    OB[3] = OB[3] + RB[3].astype(F32)
    c1.wait_recv()
    S3[0:64, :] = (total(1, 0, 64) + R1[...].astype(F32)).astype(BF16)
    c2.wait_recv()
    c3a.start()
    S4[64:128, :] = (total(2, 64, 128) + R2[...].astype(F32)).astype(BF16)
    c3b.wait_recv()
    c4b.start()
    c4a.wait_recv()
    c3a.wait_recv()
    c4b.wait_recv()
    out_ref[...] = (OB[3] + R3[...].astype(F32) + R4[...].astype(F32)).astype(BF16)
    for copy in (c1, c2, c3b, c4a, c3a, c4b):
        copy.wait_send()
    for k in range(4):
        to_other(k).wait_send()
    for d in range(1, NZ):

        @pl.when(z + d < NZ)
        def _():
            if d == 1:
                halo_copy(1).wait_send()
                halo_copy(2).wait_send()
            chain_copy(d).wait_send()


def finish(proj, qp, loc, gh, wout, par):
    vmem = pl.BlockSpec(memory_space=pltpu.VMEM)
    dma = pltpu.SemaphoreType.DMA
    block = lambda n: pltpu.VMEM((n, 2048), BF16)
    return pl.pallas_call(
        finish_kernel,
        name="finish",
        out_shape=jax.ShapeDtypeStruct((128, 2048), BF16),
        in_specs=[vmem] * 6,
        out_specs=vmem,
        scratch_shapes=[
            pltpu.VMEM((NZ, 128, LANES), BF16),
            pltpu.VMEM((2, 16, LANES), BF16),
            pltpu.VMEM((HEAD, LANES), F32),
            pltpu.VMEM((1024, 2 * LANES), BF16),
            pltpu.VMEM((4, 128, 2048), BF16),
            pltpu.VMEM((4, 128, 2048), BF16),
            pltpu.VMEM((4, 128, 2048), F32),
            block(64), block(64), block(64), block(64), block(128), block(128), block(128), block(128),
            dma((NZ,)), dma((NZ,)), dma((2,)), dma((2,)), dma((4,)), dma((4,)), dma((6,)), dma((6,)),
        ],
        compiler_params=pltpu.CompilerParams(collective_id=2, has_side_effects=True, vmem_limit_bytes=48 << 20),
        cost_estimate=pl.CostEstimate(flops=1_500_000_000, bytes_accessed=8_000_000, transcendentals=0),
    )(proj, qp, loc, gh, wout, par)


def body(
    tokens, norm_gain, w_conv_gate, w_conv_in, w_conv_value, conv_taps, w_receptance, w_key, w_value, w_decay_down,
    w_decay_up, decay_base, decay_shift, w_rate_down, w_rate_up, rate_base, key_scale, key_mix, group_gain,
    w_out_conv, w_out_state,
):
    first = lax.axis_index("tp") == 0
    low = jnp.where(first, w_decay_down, w_rate_down)
    pieces = [w.reshape(64, NY, LANES) for w in (w_conv_gate, w_conv_in, w_conv_value, w_receptance, w_key, w_value)]
    pieces.append(jnp.broadcast_to(low[:, None, :], (64, NY, LANES)))
    pieces += [w.T.reshape(64, NY, LANES) for w in (w_out_conv, w_out_state)]
    wp = jnp.concatenate(pieces, axis=2).transpose(1, 0, 2)
    par = jnp.concatenate(
        [jnp.stack([decay_base, rate_base, key_scale, key_mix, group_gain]), conv_taps], axis=0
    )
    proj, low, shift, wout = gather_and_project(tokens[0], norm_gain[None], wp, decay_shift[0])
    qp, loc, gh = block_terms(proj, low, shift, w_decay_up, w_rate_up, par)
    return finish(proj, qp, loc, gh, wout, par)[None]


def solution(mesh):
    split = Mesh(mesh.devices.reshape(NZ, NY, mesh.shape["fs"], mesh.shape["tp"]), AXES)
    placed = (
        P("fs", SP_TP, None), P(), P(SP, "tp"), P(SP, "tp"), P(SP, "tp"), P(None, "tp"), P(SP, "tp"), P(SP, "tp"),
        P(SP, "tp"), P(SP, None), P(None, "tp"), P("tp"), P("fs", SP, "tp"), P(SP, None), P(None, "tp"), P("tp"),
        P("tp"), P("tp"), P("tp"), P("tp", SP), P("tp", SP),
    )
    return jax.shard_map(
        body, mesh=split, in_specs=placed, out_specs=P("fs", SP_TP, None), check_vma=False
    )
```
